128 devices in a mesh: ep: 128 (over z, y, x, core).
Axes of the slice: x: 4, y: 4, z: 4, core: 2. Of those that a mesh axis runs over, the one named last changes fastest.
Arguments:
- hidden: bfloat16 [4096, 2048], P('ep'), may hold values from -6 to 6
- cache_keys: bfloat16 [4096, 1024, 128], P('ep'), may hold values from -512 to 512
- cache_values: bfloat16 [4096, 1024, 128], P('ep'), may hold values from -6 to 6
- lengths: int32 [4096], P('ep'), may hold values from 1 to 1024
- first_gain: float32 [2048], replicated, may hold values from 0.1 to 1.9
- query_weight: bfloat16 [2048, 1024], replicated, may hold values from -0.125 to 0.125
- key_weight: bfloat16 [2048, 128], replicated, may hold values from -0.125 to 0.125
- value_weight: bfloat16 [2048, 128], replicated, may hold values from -0.125 to 0.125
- mixing: float32 [8], replicated, may hold values from 0.3 to 0.8
- head_gain: float32 [128], replicated, may hold values from 0.1 to 1.9
- out_weight: bfloat16 [1024, 2048], replicated, may hold values from -0.1875 to 0.1875
- second_gain: float32 [2048], replicated, may hold values from 0.1 to 1.9
- routes: int32 [4096, 4], P('ep'), may hold values from 0 to 63, as said below
- route_weight: float32 [4096, 4], P('ep'), may hold values from 0.05 to 1
- expert_gate: bfloat16 [128, 2048, 256], P('ep'), may hold values from -0.125 to 0.125
- expert_up: bfloat16 [128, 2048, 256], P('ep'), may hold values from -0.125 to 0.125
- expert_down: bfloat16 [128, 256, 2048], P('ep'), may hold values from -0.25 to 0.25
Outputs:
- layer_out: bfloat16 [4096, 2048], P('ep')
- new_key: bfloat16 [4096, 128], P('ep')
- new_value: bfloat16 [4096, 128], P('ep')
The draws below stay inside these ranges and needn't reach their ends.
Inputs may be any that keep to these rules, and one draw needn't show every extreme that they name: `routes`: each row names 4 different experts of one group, that is of one block of 16 consecutive numbers. Among the rows of one device, two rows name the same set of experts or disjoint sets, and no expert is named by more than 4 rows; one and the same expert is named by exactly 4 rows on every device.
All inputs are finite; a program needn't handle non-finite values.
Results may differ from the reference program's by a relative error of at most 0.025.
Values may be sent and summed in bfloat16 or wider, within the bound.
No kernel may reach another device: no remote copies, remote signals or barrier semaphores. Data moves between devices by JAX's collectives and lax.ppermute only.
A program may use at most 128 MiB of HBM per device.

```python
import math
import jax
import jax.numpy as jnp
from jax import lax

D = 2048
HEADS = 8
DK = 64
DV = 128
D_EXPERT = 512
GROUPS = 4
EXP_SPLIT = 2
TOP_K = 4
SEQ_DEV = 32
LEN = 1024
TOKENS = 4096
EXPERTS = 64
EXP_GROUP = 16
CAP = 4


def draw_cache_keys(key, part):
    first = jax.random.fold_in(jax.random.fold_in(key, 3), 0)
    base = 1.8 * jnp.clip(jax.random.normal(first, (TOKENS, LEN, 2 * DK), jnp.float32), -6.0, 6.0)
    return base.astype(jnp.bfloat16)


def draw_routes(key, part):
    blocks = TOKENS // SEQ_DEV
    sets_group = EXP_GROUP // TOP_K
    set_count = EXPERTS // TOP_K
    tickets = set_count * CAP
    base = jax.random.fold_in(key, 7)
    star = jax.random.randint(jax.random.fold_in(base, 1), (), 0, EXPERTS).astype(jnp.int32)
    star_group = star // EXP_GROUP
    star_inner = star % EXP_GROUP

    def one_block(block_key):
        key_perm, key_order, key_rows = jax.random.split(block_key, 3)
        inner = jax.vmap(lambda part_key: jax.random.permutation(part_key, EXP_GROUP))(jax.random.split(key_perm, GROUPS)).astype(jnp.int32)
        members = inner + (jnp.arange(GROUPS, dtype=jnp.int32) * EXP_GROUP)[:, None]
        members = members.reshape(set_count, TOP_K)
        star_slot = jnp.sum(jnp.where(inner[star_group] == star_inner, jnp.arange(EXP_GROUP, dtype=jnp.int32), 0))
        star_set = star_group * sets_group + star_slot // TOP_K
        ticket_set = jnp.arange(tickets, dtype=jnp.int32) // CAP
        ranks = jax.random.permutation(key_order, tickets).astype(jnp.int32)
        sort_key = jnp.where(ticket_set == star_set, ranks - tickets, ranks)
        chosen = ticket_set[jnp.argsort(sort_key)[:SEQ_DEV]]
        rows = members[chosen]
        shuffle = jax.vmap(lambda row_key: jax.random.permutation(row_key, TOP_K))(jax.random.split(key_rows, SEQ_DEV)).astype(jnp.int32)
        return jnp.take_along_axis(rows, shuffle, axis=1)
    block_keys = jax.random.split(jax.random.fold_in(base, 2), blocks)
    return jax.vmap(one_block)(block_keys).reshape(TOKENS, TOP_K).astype(jnp.int32)


def place_ends(array, key, low, largest):
    dims = array.shape
    index_at = [jax.random.randint(jax.random.fold_in(key, axis), (), 0, dims[axis]) for axis in range(len(dims))]
    array = array.at[tuple(index_at)].set(low)
    longest = dims.index(max(dims))
    index_at[longest] = (index_at[longest] + 1) % dims[longest]
    return array.at[tuple(index_at)].set(largest)


def block_levels(own_key, shape, cuts, low, largest):
    level, own = 1.0, jax.random.fold_in(own_key, 6)
    for axis_at, shards_of in cuts:
        heights = jnp.exp(jax.random.uniform(jax.random.fold_in(own, axis_at), (shards_of,), jnp.float32, low / len(cuts), largest / len(cuts)))
        level = level * jnp.repeat(heights, shape[axis_at] // shards_of).reshape([-1 if axis == axis_at else 1 for axis in range(len(shape))])
    return level


def normal_values(stream_key, dims, deviation, limit, cuts=(), kind=jnp.bfloat16):
    entries = deviation * jax.random.normal(stream_key, dims, jnp.float32)
    if cuts:
        entries = entries * block_levels(stream_key, dims, cuts, -0.22, 0.18)
    return jnp.clip(entries, -limit, limit).astype(kind)


def setup_inputs(seed: int = 0) -> dict:
    key_of = jax.random.split(jax.random.key(seed), 18)
    hidden = normal_values(key_of[0], (TOKENS, D), 1.0, 6.0, ((0, 128),))
    cache_keys = draw_cache_keys(jax.random.fold_in(key_of[17], 71), 0)
    cache_values = normal_values(key_of[2], (TOKENS, LEN, DV), 1.0, 6.0, ((0, 128),))
    lengths = place_ends(jax.random.randint(key_of[3], (TOKENS,), 1, LEN + 1), jax.random.fold_in(key_of[3], 1), 1, LEN).astype(jnp.int32)
    first_gain = jnp.clip(1.0 + 0.18 * jax.random.normal(key_of[4], (D,), jnp.float32), 0.1, 1.9)
    query_weight = normal_values(key_of[5], (D, HEADS * 2 * DK), D ** -0.5, 0.125)
    key_weight = normal_values(key_of[6], (D, 2 * DK), D ** -0.5, 0.125)
    value_weight = normal_values(key_of[7], (D, DV), D ** -0.5, 0.125)
    mixing = jnp.clip(jax.random.uniform(key_of[8], (HEADS,), jnp.float32, 0.3, 0.8), 0.3, 0.8)
    head_gain = jnp.clip(1.0 + 0.18 * jax.random.normal(key_of[9], (DV,), jnp.float32), 0.1, 1.9)
    out_weight = normal_values(key_of[10], (HEADS * DV, D), (HEADS * DV) ** -0.5, 0.1875)
    second_gain = jnp.clip(1.0 + 0.18 * jax.random.normal(key_of[11], (D,), jnp.float32), 0.1, 1.9)
    routes = draw_routes(jax.random.fold_in(key_of[17], 71), 0)
    route_weight = jnp.clip(jnp.exp(math.log(1.0) - 2.9957323 * jax.random.uniform(key_of[13], (TOKENS, TOP_K), jnp.float32) ** block_levels(key_of[13], (TOKENS, TOP_K), ((0, 128),), -0.2, 0.2)), 0.05, 1.0)
    expert_gate = normal_values(key_of[14], (EXPERTS * EXP_SPLIT, D, D_EXPERT // EXP_SPLIT), D ** -0.5, 0.125, ((0, 128),))
    expert_up = normal_values(key_of[15], (EXPERTS * EXP_SPLIT, D, D_EXPERT // EXP_SPLIT), D ** -0.5, 0.125, ((0, 128),))
    expert_down = normal_values(key_of[16], (EXPERTS * EXP_SPLIT, D_EXPERT // EXP_SPLIT, D), D_EXPERT ** -0.5, 0.25, ((0, 128),))
    return {"hidden": hidden, "cache_keys": cache_keys, "cache_values": cache_values, "lengths": lengths, "first_gain": first_gain, "query_weight": query_weight, "key_weight": key_weight, "value_weight": value_weight, "mixing": mixing, "head_gain": head_gain, "out_weight": out_weight, "second_gain": second_gain, "routes": routes, "route_weight": route_weight, "expert_gate": expert_gate, "expert_up": expert_up, "expert_down": expert_down}


epsilon = 1e-06

def root_scale(rows, gain):
    values = rows.astype(jnp.float32)
    factor = lax.rsqrt(lax.optimization_barrier(jnp.mean(values * values, axis=-1, keepdims=True)) + epsilon)
    return values * factor * gain

def slot_tables(routes, experts, capacity):
    count, picks = routes.shape
    flat = routes.reshape(count * picks)
    indicator = (flat[:, None] == jnp.arange(experts, dtype=jnp.int32)[None, :]).astype(jnp.int32)
    before = jnp.cumsum(indicator, axis=0) - indicator
    place = lax.optimization_barrier(jnp.sum(before * indicator, axis=1))
    target = flat * capacity + place
    slots = jnp.arange(experts * capacity, dtype=jnp.int32)
    match = target[None, :] == slots[:, None]
    return match.reshape(experts * capacity, count, picks)

def attend(query, new_key, new_value, cache_keys, cache_values, lengths, mixing):
    count = query.shape[0]
    span = cache_keys.shape[1]
    queries = query.reshape(count, HEADS, 2, DK)
    keys = cache_keys.reshape(count, span, 2, DK)
    scores = jnp.einsum('shmd,slmd->shml', queries.astype(jnp.float32), keys.astype(jnp.float32)) * DK ** (-0.5)
    own_scores = jnp.einsum('shmd,smd->shm', queries.astype(jnp.float32), new_key.reshape(count, 2, DK).astype(jnp.float32)) * DK ** (-0.5)
    valid = jnp.arange(span, dtype=jnp.int32)[None, :] < lengths[:, None]
    scores = jnp.where(valid[:, None, None, :], scores, -jnp.inf)
    highest = jnp.maximum(lax.optimization_barrier(jnp.max(scores, axis=-1)), own_scores)
    weights = jnp.exp(scores - highest[..., None])
    own_weights = jnp.exp(own_scores - highest)
    total = lax.optimization_barrier(jnp.sum(weights, axis=-1)) + own_weights
    weights = weights / total[..., None]
    own_weights = own_weights / total
    contrast = (weights[:, :, 0] - mixing[None, :, None] * weights[:, :, 1]).astype(jnp.bfloat16)
    own_contrast = (own_weights[:, :, 0] - mixing[None, :] * own_weights[:, :, 1]).astype(jnp.bfloat16)
    mixed = jnp.einsum('shl,sle->she', contrast.astype(jnp.float32), cache_values.astype(jnp.float32))
    return mixed + own_contrast.astype(jnp.float32)[..., None] * new_value.astype(jnp.float32)[:, None, :]

def head_norm(mixed, head_gain):
    factor = lax.rsqrt(lax.optimization_barrier(jnp.mean(mixed * mixed, axis=-1, keepdims=True)) + epsilon)
    scaled = mixed * factor * head_gain
    return scaled.reshape(mixed.shape[0], HEADS * DV).astype(jnp.bfloat16)

def reference(hidden, cache_keys, cache_values, lengths, first_gain, query_weight, key_weight, value_weight, mixing, head_gain, out_weight, second_gain, routes, route_weight, expert_gate, expert_up, expert_down):
    normed = root_scale(hidden, first_gain).astype(jnp.bfloat16)
    query = jnp.dot(normed, query_weight, preferred_element_type=jnp.float32).astype(jnp.bfloat16)
    new_key = jnp.dot(normed, key_weight, preferred_element_type=jnp.float32).astype(jnp.bfloat16)
    new_value = jnp.dot(normed, value_weight, preferred_element_type=jnp.float32).astype(jnp.bfloat16)
    mixed = attend(query, new_key, new_value, cache_keys, cache_values, lengths, mixing)
    head_rows = head_norm(mixed, head_gain)
    update = jnp.dot(head_rows, out_weight, preferred_element_type=jnp.float32)
    residual = (hidden.astype(jnp.float32) + update).astype(jnp.bfloat16)
    expert_input = root_scale(residual, second_gain).astype(jnp.bfloat16)
    blocks = TOKENS // SEQ_DEV
    match = jax.vmap(lambda block: slot_tables(block, EXPERTS, CAP))(routes.reshape(blocks, SEQ_DEV, TOP_K))
    pick = lax.optimization_barrier(jnp.sum(match.astype(jnp.float32), axis=3))
    packed = jnp.einsum('bjs,bsd->bjd', pick, expert_input.reshape(blocks, SEQ_DEV, D).astype(jnp.float32))
    packed = packed.astype(jnp.bfloat16).reshape(blocks, EXPERTS, CAP, D)

    def one_expert(index):
        rows = lax.dynamic_index_in_dim(packed, index, 1, keepdims=False).reshape(blocks * CAP, D)
        summed = jnp.zeros((blocks * CAP, D), jnp.float32)
        for share in range(EXP_SPLIT):
            part = index * EXP_SPLIT + share
            gate = jnp.dot(rows, expert_gate[part], preferred_element_type=jnp.float32)
            upper = jnp.dot(rows, expert_up[part], preferred_element_type=jnp.float32)
            inner = (jax.nn.silu(gate) * upper).astype(jnp.bfloat16)
            result = jnp.dot(inner, expert_down[part], preferred_element_type=jnp.float32).astype(jnp.bfloat16)
            summed = summed + result.astype(jnp.float32)
        return summed.reshape(blocks, CAP, D)
    outputs = lax.map(one_expert, jnp.arange(EXPERTS, dtype=jnp.int32))
    outputs = jnp.moveaxis(outputs, 0, 1).reshape(blocks, EXPERTS * CAP, D)
    weighting = lax.optimization_barrier(jnp.sum(jnp.where(match, route_weight.reshape(blocks, 1, SEQ_DEV, TOP_K), 0.0), axis=3))
    routed = jnp.einsum('bjs,bjd->bsd', weighting, outputs, precision=lax.Precision.HIGHEST)
    layer_out = (residual.astype(jnp.float32) + routed.reshape(TOKENS, D)).astype(jnp.bfloat16)
    return (layer_out, new_key, new_value)
```

```python
import jax
import jax.numpy as jnp
from jax import lax
from jax.experimental import pallas as pl
from jax.experimental.pallas import tpu as pltpu
from jax.sharding import PartitionSpec as P

D = 2048
HALF = D // 2
HEADS = 8
DK = 64
DV = 128
EXP_SPLIT = 2
TOP_K = 4
CAP = 4
ROWS = 8
BLOCK = 256
GROUP = 4
WCHUNKS = 4

epsilon = 1e-06
MIB = 1024 * 1024


def root_factor(values):
    return lax.rsqrt(jnp.mean(values * values, axis=-1, keepdims=True) + epsilon)


def routing_tables(routes, route_weight, pick, weighting_out):
    count = routes.shape[1]
    slots = pick.shape[0]
    f32 = jnp.float32
    across = [routes[j : j + 1, :].astype(f32) for j in range(TOP_K)]
    rows_at = lax.broadcasted_iota(jnp.int32, (count, count), 0)
    columns_at = lax.broadcasted_iota(jnp.int32, (count, count), 1)

    def turn(row):
        return jnp.sum(jnp.where(rows_at == columns_at, row, 0.0), axis=1, keepdims=True)

    down = [turn(row) for row in across]
    same = down[0] == across[0]
    for j in range(1, TOP_K):
        same = same | (down[0] == across[j])
    shared = jnp.where(same, 1.0, 0.0)
    rank_across = jnp.sum(jnp.where(rows_at < columns_at, shared, 0.0), axis=0, keepdims=True)
    rank_down = turn(rank_across)

    slot = lax.broadcasted_iota(jnp.int32, (slots, count), 0)
    expert = (slot // ROWS).astype(f32)
    hit = expert == across[0]
    for j in range(1, TOP_K):
        hit = hit | (expert == across[j])
    chosen = jnp.where(hit & ((slot % CAP).astype(f32) == rank_across), 1.0, 0.0)
    upper = (slot // CAP) % 2 == 1
    pick[...] = jnp.concatenate(
        [jnp.where(upper, 0.0, chosen), jnp.where(upper, chosen, 0.0)], axis=1
    ).astype(jnp.bfloat16)

    slot = lax.broadcasted_iota(jnp.int32, (count, slots), 1)
    expert = (slot // ROWS).astype(f32)
    weighting = jnp.zeros((count, slots), f32)
    for j in range(TOP_K):
        weighting = weighting + jnp.where(
            expert == down[j], turn(route_weight[j : j + 1, :]), 0.0
        )
    weighting = jnp.where((slot % CAP).astype(f32) == rank_down, weighting, 0.0)
    upper = (slot // CAP) % 2 == 1
    whole = jnp.concatenate(
        [jnp.where(upper, 0.0, weighting), jnp.where(upper, weighting, 0.0)], axis=0
    )
    coarse = whole.astype(jnp.bfloat16)
    fine = (whole - coarse.astype(f32)).astype(jnp.bfloat16)
    weighting_out[...] = jnp.concatenate([coarse, fine], axis=0)


def front_kernel(
    lengths_hbm,
    mixing_hbm,
    hidden_hbm,
    first_gain_hbm,
    head_gain_hbm,
    second_gain_hbm,
    routes_hbm,
    route_weight_hbm,
    wq_hbm,
    wk_hbm,
    wv_hbm,
    wo_hbm,
    keys_hbm,
    values_hbm,
    packed,
    residual_out,
    new_key_out,
    new_value_out,
    weighting_out,
    lengths,
    mixing,
    hidden,
    first_gain,
    head_gain,
    second_gain,
    routes,
    route_weight,
    wq,
    wk,
    wv,
    wo,
    kbuf,
    vbuf,
    queries,
    own_key,
    own_value,
    mixed,
    pick,
    order,
    ssem,
    wsem,
    osem,
    ksem,
    vsem,
):
    count = hidden.shape[0]
    span = keys_hbm.shape[1]
    blocks = span // BLOCK
    groups = count // GROUP
    part = D // WCHUNKS

    def weight_copies(i):
        rows = pl.ds(i * part, part)
        return [
            pltpu.make_async_copy(source.at[rows], target.at[rows], wsem.at[n, i])
            for n, (source, target) in enumerate(((wq_hbm, wq), (wk_hbm, wk), (wv_hbm, wv)))
        ]

    small = [
        pltpu.make_async_copy(source, target, ssem.at[n])
        for n, (source, target) in enumerate(
            (
                (lengths_hbm, lengths),
                (hidden_hbm, hidden),
                (first_gain_hbm, first_gain),
                (routes_hbm, routes),
                (route_weight_hbm, route_weight),
                (mixing_hbm, mixing),
                (head_gain_hbm, head_gain),
                (second_gain_hbm, second_gain),
            )
        )
    ]
    for copy in small:
        copy.start()
    for i in range(WCHUNKS):
        for copy in weight_copies(i):
            copy.start()
    small[0].wait()

    def blocks_of(i):
        return (lengths[i] + (BLOCK - 1)) // BLOCK

    place = jnp.int32(0)
    for b in range(1, blocks + 1):
        for i in range(count):
            order[place] = jnp.int32(i)
            place = place + (blocks_of(i) == b).astype(jnp.int32)

    def cache_copies(g, n):
        copies = []
        rows = pl.ds(0, n * BLOCK)
        for i in range(GROUP):
            at = g * GROUP + i
            s = order[at]
            copies.append(
                pltpu.make_async_copy(keys_hbm.at[s, rows], kbuf.at[at, rows], ksem.at[at])
            )
            copies.append(
                pltpu.make_async_copy(values_hbm.at[s, rows], vbuf.at[at, rows], vsem.at[at])
            )
        return copies

    def start_group(g, carry):
        need = blocks_of(order[g * GROUP + GROUP - 1])
        for n in range(1, blocks + 1):

            @pl.when(need == n)
            def _():
                for copy in cache_copies(g, n):
                    copy.start()

        return carry

    lax.fori_loop(0, groups, start_group, 0)
    wo_copy = pltpu.make_async_copy(wo_hbm, wo, osem)
    wo_copy.start()
    for copy in small[1:]:
        copy.wait()
    routing_tables(routes, route_weight, pick, weighting_out)

    hid = hidden[...].astype(jnp.float32)
    normed = (hid * root_factor(hid) * first_gain[...]).astype(jnp.bfloat16)
    q = jnp.zeros((count, HEADS * 2 * DK), jnp.float32)
    k = jnp.zeros((count, 2 * DK), jnp.float32)
    v = jnp.zeros((count, DV), jnp.float32)
    for i in range(WCHUNKS):
        for copy in weight_copies(i):
            copy.wait()
        rows = slice(i * part, (i + 1) * part)
        left = normed[:, rows]
        q = q + jnp.dot(left, wq[rows], preferred_element_type=jnp.float32)
        k = k + jnp.dot(left, wk[rows], preferred_element_type=jnp.float32)
        v = v + jnp.dot(left, wv[rows], preferred_element_type=jnp.float32)
    q = q.astype(jnp.bfloat16).astype(jnp.float32) * DK ** (-0.5)
    k = k.astype(jnp.bfloat16)
    v = v.astype(jnp.bfloat16)
    new_key_out[...] = k
    new_value_out[...] = v
    own_key[...] = k.astype(jnp.float32)
    own_value[...] = v.astype(jnp.float32)
    for h in range(HEADS):
        queries[pl.ds(h, count, stride=HEADS), :] = q[:, h * 2 * DK : (h + 1) * 2 * DK]

    head_at = lax.broadcasted_iota(jnp.int32, (HEADS, 1), 0)
    mix = jnp.zeros((HEADS, 1), jnp.float32)
    for h in range(HEADS):
        mix = jnp.where(head_at == h, mixing[h], mix)
    low = lax.broadcasted_iota(jnp.int32, (HEADS, 2 * DK), 1) < DK

    def attend_group(g, n):
        for copy in cache_copies(g, n):
            copy.wait()
        wide = n * BLOCK
        column = lax.broadcasted_iota(jnp.int32, (2 * HEADS, wide), 1)
        for i in range(GROUP):
            at = g * GROUP + i
            s = order[at]
            rows = queries[pl.ds(pl.multiple_of(s * HEADS, HEADS), HEADS), :]
            both = jnp.concatenate([jnp.where(low, rows, 0.0), jnp.where(low, 0.0, rows)], axis=0)
            own = jnp.sum(both * own_key[pl.ds(s, 1), :], axis=-1, keepdims=True)
            scores = lax.dot_general(
                both.astype(jnp.bfloat16),
                kbuf[at, :wide, :],
                (((1,), (1,)), ((), ())),
                preferred_element_type=jnp.float32,
            )
            scores = jnp.where(column < lengths[s], scores, -jnp.inf)
            highest = jnp.maximum(jnp.max(scores, axis=-1, keepdims=True), own)
            weights = jnp.exp(scores - highest)
            own_weights = jnp.exp(own - highest)
            total = jnp.sum(weights, axis=-1, keepdims=True) + own_weights
            first = 1.0 / total[:HEADS]
            second = mix / total[HEADS:]
            contrast = (weights[:HEADS] * first - weights[HEADS:] * second).astype(jnp.bfloat16)
            own_contrast = (own_weights[:HEADS] * first - own_weights[HEADS:] * second).astype(
                jnp.bfloat16
            )
            out = jnp.dot(contrast, vbuf[at, :wide, :], preferred_element_type=jnp.float32)
            out = out + own_contrast.astype(jnp.float32) * own_value[pl.ds(s, 1), :]
            mixed[pl.ds(pl.multiple_of(s * HEADS, HEADS), HEADS), :] = out

    def run_group(g, carry):
        need = blocks_of(order[g * GROUP + GROUP - 1])
        for n in range(1, blocks + 1):

            @pl.when(need == n)
            def _():
                attend_group(g, n)

        return carry

    lax.fori_loop(0, groups, run_group, 0)

    pieces = []
    for h in range(HEADS):
        rows = mixed[pl.ds(h, count, stride=HEADS), :]
        pieces.append((rows * root_factor(rows) * head_gain[...]).astype(jnp.bfloat16))
    head_rows = jnp.concatenate(pieces, axis=1)
    wo_copy.wait()
    update = jnp.dot(head_rows, wo[...], preferred_element_type=jnp.float32)
    residual = (hid + update).astype(jnp.bfloat16)
    residual_out[...] = residual
    res = residual.astype(jnp.float32)
    expert_input = (res * root_factor(res) * second_gain[...]).astype(jnp.bfloat16)

    stacked = jnp.concatenate([expert_input[:, :HALF], expert_input[:, HALF:]], axis=0)
    sent = jnp.dot(pick[...], stacked, preferred_element_type=jnp.float32).astype(jnp.bfloat16)
    packed[...] = sent.reshape(packed.shape)


def front(
    lengths,
    mixing,
    hidden,
    first_gain,
    head_gain,
    second_gain,
    routes,
    route_weight,
    wq,
    wk,
    wv,
    wo,
    keys,
    values,
    experts,
):
    count = hidden.shape[0]
    slots = experts * ROWS
    vmem = pl.BlockSpec(memory_space=pltpu.VMEM)
    hbm = pl.BlockSpec(memory_space=pltpu.HBM)
    bf16 = jnp.bfloat16
    f32 = jnp.float32
    operands = (
        lengths,
        mixing,
        hidden,
        first_gain.reshape(1, D),
        head_gain.reshape(1, DV),
        second_gain.reshape(1, D),
        routes.T,
        route_weight.T,
        wq,
        wk,
        wv,
        wo,
        keys,
        values,
    )
    return pl.pallas_call(
        front_kernel,
        out_shape=(
            jax.ShapeDtypeStruct((experts, ROWS, HALF), bf16),
            jax.ShapeDtypeStruct((count, D), bf16),
            jax.ShapeDtypeStruct((count, 2 * DK), bf16),
            jax.ShapeDtypeStruct((count, DV), bf16),
            jax.ShapeDtypeStruct((4 * count, slots), bf16),
        ),
        in_specs=[hbm] * 14,
        out_specs=(vmem,) * 5,
        scratch_shapes=[
            pltpu.SMEM(lengths.shape, jnp.int32),
            pltpu.SMEM(mixing.shape, f32),
            pltpu.VMEM(hidden.shape, bf16),
            pltpu.VMEM((1, D), f32),
            pltpu.VMEM((1, DV), f32),
            pltpu.VMEM((1, D), f32),
            pltpu.VMEM((TOP_K, count), jnp.int32),
            pltpu.VMEM((TOP_K, count), f32),
            pltpu.VMEM(wq.shape, bf16),
            pltpu.VMEM(wk.shape, bf16),
            pltpu.VMEM(wv.shape, bf16),
            pltpu.VMEM(wo.shape, bf16),
            pltpu.VMEM(keys.shape, bf16),
            pltpu.VMEM(values.shape, bf16),
            pltpu.VMEM((count * HEADS, 2 * DK), f32),
            pltpu.VMEM((count, 2 * DK), f32),
            pltpu.VMEM((count, DV), f32),
            pltpu.VMEM((count * HEADS, DV), f32),
            pltpu.VMEM((slots, 2 * count), bf16),
            pltpu.SMEM((count + 1,), jnp.int32),
            pltpu.SemaphoreType.DMA((8,)),
            pltpu.SemaphoreType.DMA((3, WCHUNKS)),
            pltpu.SemaphoreType.DMA(()),
            pltpu.SemaphoreType.DMA((count,)),
            pltpu.SemaphoreType.DMA((count,)),
        ],
        compiler_params=pltpu.CompilerParams(vmem_limit_bytes=40 * MIB),
        cost_estimate=pl.CostEstimate(
            flops=20_000_000_000, transcendentals=0, bytes_accessed=25 * MIB
        ),
        name="front",
    )(*[pltpu.with_memory_space_constraint(x, pltpu.HBM) for x in operands])


def swap_halves(pairs):
    first = pairs[:, 0]
    second = pairs[:, 1]
    top = lax.broadcasted_iota(jnp.int32, first.shape, 1) < CAP
    low = jnp.where(top, first, pltpu.roll(second, CAP, 1))
    high = jnp.where(top, pltpu.roll(first, CAP, 1), second)
    return low, high


def expert_kernel(rows, gate_a, gate_b, up_a, up_b, down_a, down_b, result):
    sources = rows.shape[0]
    count = sources * CAP
    f32 = jnp.float32
    pairs = rows[...].astype(f32).reshape(sources // 2, 2, ROWS, HALF)
    low, high = swap_halves(pairs)
    low = low.reshape(count, HALF).astype(jnp.bfloat16)
    high = high.reshape(count, HALF).astype(jnp.bfloat16)

    def project(weight):
        return jnp.dot(low, weight[:HALF], preferred_element_type=f32) + jnp.dot(
            high, weight[HALF:], preferred_element_type=f32
        )

    inner = []
    for gate_w, up_w in ((gate_a, up_a), (gate_b, up_b)):
        gate = project(gate_w)
        inner.append((gate / (1.0 + jnp.exp(-gate)) * project(up_w)).astype(jnp.bfloat16))
    halves = []
    for j in range(2):
        columns = slice(j * HALF, (j + 1) * HALF)
        half = jnp.dot(inner[0], down_a[:, columns], preferred_element_type=f32) + jnp.dot(
            inner[1], down_b[:, columns], preferred_element_type=f32
        )
        halves.append(half.reshape(sources // 2, 1, ROWS, HALF))
    first, second = swap_halves(jnp.concatenate(halves, axis=1))
    result[...] = (
        jnp.stack([first, second], axis=1).reshape(sources, ROWS, HALF).astype(jnp.bfloat16)
    )


def expert(rows, *weights):
    return pl.pallas_call(
        expert_kernel,
        out_shape=jax.ShapeDtypeStruct(rows.shape, rows.dtype),
        compiler_params=pltpu.CompilerParams(vmem_limit_bytes=32 * MIB),
        cost_estimate=pl.CostEstimate(
            flops=3_000_000_000, transcendentals=0, bytes_accessed=8 * MIB
        ),
        name="expert",
    )(rows, *weights)


def combine_kernel(returned, residual, weighting, out):
    count = residual.shape[0]
    values = returned[...].reshape(returned.shape[0] * ROWS, HALF)
    both = jnp.dot(weighting[...], values, preferred_element_type=jnp.float32)
    routed = both[: 2 * count] + both[2 * count :]
    res = residual[...].astype(jnp.float32)
    out[:, :HALF] = (res[:, :HALF] + routed[:count]).astype(jnp.bfloat16)
    out[:, HALF:] = (res[:, HALF:] + routed[count:]).astype(jnp.bfloat16)


def combine(returned, residual, weighting):
    return pl.pallas_call(
        combine_kernel,
        out_shape=jax.ShapeDtypeStruct(residual.shape, residual.dtype),
        compiler_params=pltpu.CompilerParams(vmem_limit_bytes=16 * MIB),
        name="combine",
    )(returned, residual, weighting)


def per_device(
    hidden,
    cache_keys,
    cache_values,
    lengths,
    first_gain,
    query_weight,
    key_weight,
    value_weight,
    mixing,
    head_gain,
    out_weight,
    second_gain,
    routes,
    route_weight,
    expert_gate,
    expert_up,
    expert_down,
):
    devices = lax.axis_size("ep")
    experts = devices // EXP_SPLIT
    partners = [(i, i ^ 1) for i in range(devices)]
    lanes = [[e * EXP_SPLIT + j for e in range(experts)] for j in range(EXP_SPLIT)]
    peer = [lax.ppermute(w[0], "ep", partners) for w in (expert_gate, expert_up, expert_down)]

    packed, residual, new_key, new_value, weighting = front(
        lengths,
        mixing,
        hidden,
        first_gain,
        head_gain,
        second_gain,
        routes,
        route_weight,
        query_weight,
        key_weight,
        value_weight,
        out_weight,
        cache_keys,
        cache_values,
        experts,
    )
    rows = lax.all_to_all(packed, "ep", 0, 0, axis_index_groups=lanes, tiled=True)
    result = expert(
        rows, expert_gate[0], peer[0], expert_up[0], peer[1], expert_down[0], peer[2]
    )
    returned = lax.all_to_all(result, "ep", 0, 0, axis_index_groups=lanes, tiled=True)
    layer_out = combine(returned, residual, weighting)
    return (layer_out, new_key, new_value)


def solution(mesh):
    return jax.shard_map(
        per_device,
        mesh=mesh,
        in_specs=(
            P("ep", None),
            P("ep", None, None),
            P("ep", None, None),
            P("ep"),
            P(),
            P(),
            P(),
            P(),
            P(),
            P(),
            P(),
            P(),
            P("ep", None),
            P("ep", None),
            P("ep", None, None),
            P("ep", None, None),
            P("ep", None, None),
        ),
        out_specs=(P("ep", None), P("ep", None), P("ep", None)),
        check_vma=False,
    )
```

```python
import jax
import jax.numpy as jnp
from jax import lax
from jax.experimental import pallas as pl
from jax.experimental.pallas import tpu as pltpu
from jax.sharding import PartitionSpec as P

D = 2048
HALF = D // 2
HEADS = 8
DK = 64
DV = 128
EXP_SPLIT = 2
TOP_K = 4
CAP = 4
ROWS = 8
BLOCK = 256
GROUP = 8
WCHUNKS = 4

epsilon = 1e-06
MIB = 1024 * 1024


def root_factor(values):
    return lax.rsqrt(jnp.mean(values * values, axis=-1, keepdims=True) + epsilon)


def routing_tables(routes, route_weight, pick, weighting_out):
    count = routes.shape[1]
    slots = pick.shape[0]
    f32 = jnp.float32
    across = [routes[j : j + 1, :].astype(f32) for j in range(TOP_K)]
    rows_at = lax.broadcasted_iota(jnp.int32, (count, count), 0)
    columns_at = lax.broadcasted_iota(jnp.int32, (count, count), 1)

    def turn(row):
        return jnp.sum(jnp.where(rows_at == columns_at, row, 0.0), axis=1, keepdims=True)

    down = [turn(row) for row in across]
    same = down[0] == across[0]
    for j in range(1, TOP_K):
        same = same | (down[0] == across[j])
    shared = jnp.where(same, 1.0, 0.0)
    rank_across = jnp.sum(jnp.where(rows_at < columns_at, shared, 0.0), axis=0, keepdims=True)
    rank_down = turn(rank_across)

    slot = lax.broadcasted_iota(jnp.int32, (slots, count), 0)
    expert = (slot // ROWS).astype(f32)
    hit = expert == across[0]
    for j in range(1, TOP_K):
        hit = hit | (expert == across[j])
    chosen = jnp.where(hit & ((slot % CAP).astype(f32) == rank_across), 1.0, 0.0)
    upper = (slot // CAP) % 2 == 1
    pick[...] = jnp.concatenate(
        [jnp.where(upper, 0.0, chosen), jnp.where(upper, chosen, 0.0)], axis=1
    ).astype(jnp.bfloat16)

    slot = lax.broadcasted_iota(jnp.int32, (count, slots), 1)
    expert = (slot // ROWS).astype(f32)
    weighting = jnp.zeros((count, slots), f32)
    for j in range(TOP_K):
        weighting = weighting + jnp.where(
            expert == down[j], turn(route_weight[j : j + 1, :]), 0.0
        )
    weighting = jnp.where((slot % CAP).astype(f32) == rank_down, weighting, 0.0)
    upper = (slot // CAP) % 2 == 1
    whole = jnp.concatenate(
        [jnp.where(upper, 0.0, weighting), jnp.where(upper, weighting, 0.0)], axis=0
    )
    coarse = whole.astype(jnp.bfloat16)
    fine = (whole - coarse.astype(f32)).astype(jnp.bfloat16)
    weighting_out[...] = jnp.concatenate([coarse, fine], axis=0)


def front_kernel(
    lengths_hbm,
    mixing_hbm,
    hidden_hbm,
    first_gain_hbm,
    head_gain_hbm,
    second_gain_hbm,
    routes_hbm,
    route_weight_hbm,
    wq_hbm,
    wk_hbm,
    wv_hbm,
    wo_hbm,
    keys_hbm,
    values_hbm,
    packed,
    residual_out,
    new_key_out,
    new_value_out,
    weighting_out,
    lengths,
    mixing,
    hidden,
    first_gain,
    head_gain,
    second_gain,
    routes,
    route_weight,
    wq,
    wk,
    wv,
    wo,
    kbuf,
    vbuf,
    queries,
    own_key,
    own_value,
    mixed,
    own_scores,
    scores_at,
    pick,
    order,
    ssem,
    wsem,
    osem,
    ksem,
    vsem,
):
    count = hidden.shape[0]
    span = keys_hbm.shape[1]
    blocks = span // BLOCK
    groups = count // GROUP
    part = D // WCHUNKS

    def weight_copies(i):
        rows = pl.ds(i * part, part)
        return [
            pltpu.make_async_copy(source.at[rows], target.at[rows], wsem.at[n, i])
            for n, (source, target) in enumerate(((wq_hbm, wq), (wk_hbm, wk), (wv_hbm, wv)))
        ]

    small = [
        pltpu.make_async_copy(source, target, ssem.at[n])
        for n, (source, target) in enumerate(
            (
                (lengths_hbm, lengths),
                (hidden_hbm, hidden),
                (first_gain_hbm, first_gain),
                (routes_hbm, routes),
                (route_weight_hbm, route_weight),
                (mixing_hbm, mixing),
                (head_gain_hbm, head_gain),
                (second_gain_hbm, second_gain),
            )
        )
    ]
    for copy in small:
        copy.start()
    for i in range(WCHUNKS):
        for copy in weight_copies(i):
            copy.start()
    small[0].wait()

    def passed(i):
        return [(lengths[i] > b * BLOCK).astype(jnp.int32) for b in range(1, blocks)]

    starts = [jnp.int32(0)] + [jnp.int32(count)] * (blocks - 1)
    for i in range(count):
        more = passed(i)
        starts = starts[:1] + [at - one for at, one in zip(starts[1:], more)]
    for i in range(count):
        more = passed(i)
        place = starts[0]
        for at, one in zip(starts[1:], more):
            place = jnp.where(one > 0, at, place)
        order[place] = jnp.int32(i)
        kinds = [1] + more + [0]
        starts = [at + (kinds[b] - kinds[b + 1]) for b, at in enumerate(starts)]

    def group_blocks(g):
        return 1 + sum(passed(order[g * GROUP + GROUP - 1]))

    def cache_copies(source, target, sem, g, n):
        rows = pl.ds(0, n * BLOCK)
        return [
            pltpu.make_async_copy(
                source.at[order[g * GROUP + i], rows],
                target.at[g * GROUP + i, rows],
                sem.at[g * GROUP + i],
            )
            for i in range(GROUP)
        ]

    def by_blocks(body):
        def step(g, carry):
            need = group_blocks(g)
            for n in range(1, blocks + 1):

                @pl.when(need == n)
                def _():
                    body(g, n)

            return carry

        lax.fori_loop(0, groups, step, 0)

    def start_keys(g, n):
        for copy in cache_copies(keys_hbm, kbuf, ksem, g, n):
            copy.start()

    def start_values(g, n):
        for copy in cache_copies(values_hbm, vbuf, vsem, g, n):
            copy.start()

    by_blocks(start_keys)
    by_blocks(start_values)
    wo_copy = pltpu.make_async_copy(wo_hbm, wo, osem)
    wo_copy.start()
    for copy in small[1:]:
        copy.wait()
    routing_tables(routes, route_weight, pick, weighting_out)

    hid = hidden[...].astype(jnp.float32)
    normed = (hid * root_factor(hid) * first_gain[...]).astype(jnp.bfloat16)
    q = jnp.zeros((count, HEADS * 2 * DK), jnp.float32)
    k = jnp.zeros((count, 2 * DK), jnp.float32)
    v = jnp.zeros((count, DV), jnp.float32)
    for i in range(WCHUNKS):
        for copy in weight_copies(i):
            copy.wait()
        rows = slice(i * part, (i + 1) * part)
        left = normed[:, rows]
        q = q + jnp.dot(left, wq[rows], preferred_element_type=jnp.float32)
        k = k + jnp.dot(left, wk[rows], preferred_element_type=jnp.float32)
        v = v + jnp.dot(left, wv[rows], preferred_element_type=jnp.float32)
    q = q.astype(jnp.bfloat16).astype(jnp.float32) * DK ** (-0.5)
    k = k.astype(jnp.bfloat16)
    v = v.astype(jnp.bfloat16)
    new_key_out[...] = k
    new_value_out[...] = v
    own_key[...] = k.astype(jnp.float32)
    own_value[...] = v.astype(jnp.float32)
    for h in range(HEADS):
        queries[pl.ds(h, count, stride=HEADS), :] = q[:, h * 2 * DK : (h + 1) * 2 * DK]

    head_at = lax.broadcasted_iota(jnp.int32, (HEADS, 1), 0)
    mix = jnp.zeros((HEADS, 1), jnp.float32)
    for h in range(HEADS):
        mix = jnp.where(head_at == h, mixing[h], mix)
    low = lax.broadcasted_iota(jnp.int32, (HEADS, 2 * DK), 1) < DK
    pair = 2 * HEADS
    lane_owner = lax.broadcasted_iota(jnp.int32, (2 * DK, GROUP * pair), 1) // pair

    def score_group(g, n):
        wide = n * BLOCK
        both = []
        for i in range(GROUP):
            s = order[g * GROUP + i]
            rows = queries[pl.ds(pl.multiple_of(s * HEADS, HEADS), HEADS), :]
            both.append(
                jnp.concatenate([jnp.where(low, rows, 0.0), jnp.where(low, 0.0, rows)], axis=0)
            )
            own_rows = both[i] * own_key[pl.ds(s, 1), :]
            own_scores[g, i * pair : (i + 1) * pair, :] = own_rows
        turned = jnp.concatenate(both, axis=0).T
        spread = jnp.concatenate(
            [jnp.where(lane_owner == i, turned, 0.0) for i in range(GROUP)], axis=0
        ).astype(jnp.bfloat16)
        for copy in cache_copies(keys_hbm, kbuf, ksem, g, n):
            copy.wait()
        keys = jnp.concatenate([kbuf[g * GROUP + i, :wide, :] for i in range(GROUP)], axis=1)
        scores_at[g, :, :wide] = jnp.dot(keys, spread, preferred_element_type=jnp.float32).T

    def mix_group(g, n):
        wide = n * BLOCK
        column = lax.broadcasted_iota(jnp.int32, (pair, wide), 1)
        for copy in cache_copies(values_hbm, vbuf, vsem, g, n):
            copy.wait()
        for i in range(GROUP):
            s = order[g * GROUP + i]
            rows = slice(i * pair, (i + 1) * pair)
            own = jnp.sum(own_scores[g, rows, :], axis=-1, keepdims=True)
            scores = jnp.where(column < lengths[s], scores_at[g, rows, :wide], -jnp.inf)
            highest = jnp.maximum(jnp.max(scores, axis=-1, keepdims=True), own)
            weights = jnp.exp(scores - highest)
            own_weights = jnp.exp(own - highest)
            total = jnp.sum(weights, axis=-1, keepdims=True) + own_weights
            first = 1.0 / total[:HEADS]
            second = mix / total[HEADS:]
            contrast = (weights[:HEADS] * first - weights[HEADS:] * second).astype(jnp.bfloat16)
            own_contrast = (own_weights[:HEADS] * first - own_weights[HEADS:] * second).astype(
                jnp.bfloat16
            )
            out = jnp.dot(
                contrast, vbuf[g * GROUP + i, :wide, :], preferred_element_type=jnp.float32
            )
            out = out + own_contrast.astype(jnp.float32) * own_value[pl.ds(s, 1), :]
            mixed[pl.ds(pl.multiple_of(s * HEADS, HEADS), HEADS), :] = out

    by_blocks(score_group)
    by_blocks(mix_group)

    pieces = []
    for h in range(HEADS):
        rows = mixed[pl.ds(h, count, stride=HEADS), :]
        pieces.append((rows * root_factor(rows) * head_gain[...]).astype(jnp.bfloat16))
    head_rows = jnp.concatenate(pieces, axis=1)
    wo_copy.wait()
    update = jnp.dot(head_rows, wo[...], preferred_element_type=jnp.float32)
    residual = (hid + update).astype(jnp.bfloat16)
    residual_out[...] = residual
    res = residual.astype(jnp.float32)
    expert_input = (res * root_factor(res) * second_gain[...]).astype(jnp.bfloat16)

    stacked = jnp.concatenate([expert_input[:, :HALF], expert_input[:, HALF:]], axis=0)
    sent = jnp.dot(pick[...], stacked, preferred_element_type=jnp.float32).astype(jnp.bfloat16)
    packed[...] = sent.reshape(packed.shape)


def front(
    lengths,
    mixing,
    hidden,
    first_gain,
    head_gain,
    second_gain,
    routes,
    route_weight,
    wq,
    wk,
    wv,
    wo,
    keys,
    values,
    experts,
):
    count = hidden.shape[0]
    slots = experts * ROWS
    vmem = pl.BlockSpec(memory_space=pltpu.VMEM)
    hbm = pl.BlockSpec(memory_space=pltpu.HBM)
    bf16 = jnp.bfloat16
    f32 = jnp.float32
    operands = (
        lengths,
        mixing,
        hidden,
        first_gain.reshape(1, D),
        head_gain.reshape(1, DV),
        second_gain.reshape(1, D),
        routes.T,
        route_weight.T,
        wq,
        wk,
        wv,
        wo,
        keys,
        values,
    )
    return pl.pallas_call(
        front_kernel,
        out_shape=(
            jax.ShapeDtypeStruct((experts, ROWS, HALF), bf16),
            jax.ShapeDtypeStruct((count, D), bf16),
            jax.ShapeDtypeStruct((count, 2 * DK), bf16),
            jax.ShapeDtypeStruct((count, DV), bf16),
            jax.ShapeDtypeStruct((4 * count, slots), bf16),
        ),
        in_specs=[hbm] * 14,
        out_specs=(vmem,) * 5,
        scratch_shapes=[
            pltpu.SMEM(lengths.shape, jnp.int32),
            pltpu.SMEM(mixing.shape, f32),
            pltpu.VMEM(hidden.shape, bf16),
            pltpu.VMEM((1, D), f32),
            pltpu.VMEM((1, DV), f32),
            pltpu.VMEM((1, D), f32),
            pltpu.VMEM((TOP_K, count), jnp.int32),
            pltpu.VMEM((TOP_K, count), f32),
            pltpu.VMEM(wq.shape, bf16),
            pltpu.VMEM(wk.shape, bf16),
            pltpu.VMEM(wv.shape, bf16),
            pltpu.VMEM(wo.shape, bf16),
            pltpu.VMEM(keys.shape, bf16),
            pltpu.VMEM(values.shape, bf16),
            pltpu.VMEM((count * HEADS, 2 * DK), f32),
            pltpu.VMEM((count, 2 * DK), f32),
            pltpu.VMEM((count, DV), f32),
            pltpu.VMEM((count * HEADS, DV), f32),
            pltpu.VMEM((count // GROUP, GROUP * 2 * HEADS, 2 * DK), f32),
            pltpu.VMEM((count // GROUP, GROUP * 2 * HEADS, keys.shape[1]), f32),
            pltpu.VMEM((slots, 2 * count), bf16),
            pltpu.SMEM((count + 1,), jnp.int32),
            pltpu.SemaphoreType.DMA((8,)),
            pltpu.SemaphoreType.DMA((3, WCHUNKS)),
            pltpu.SemaphoreType.DMA(()),
            pltpu.SemaphoreType.DMA((count,)),
            pltpu.SemaphoreType.DMA((count,)),
        ],
        compiler_params=pltpu.CompilerParams(vmem_limit_bytes=40 * MIB),
        cost_estimate=pl.CostEstimate(
            flops=20_000_000_000, transcendentals=0, bytes_accessed=25 * MIB
        ),
        name="front",
    )(*[pltpu.with_memory_space_constraint(x, pltpu.HBM) for x in operands])


def swap_halves(pairs):
    first = pairs[:, 0]
    second = pairs[:, 1]
    top = lax.broadcasted_iota(jnp.int32, first.shape, 1) < CAP
    low = jnp.where(top, first, pltpu.roll(second, CAP, 1))
    high = jnp.where(top, pltpu.roll(first, CAP, 1), second)
    return low, high


def expert_kernel(rows, gate_a, gate_b, up_a, up_b, down_a, down_b, result):
    sources = rows.shape[0]
    count = sources * CAP
    f32 = jnp.float32
    pairs = rows[...].astype(f32).reshape(sources // 2, 2, ROWS, HALF)
    low, high = swap_halves(pairs)
    low = low.reshape(count, HALF).astype(jnp.bfloat16)
    high = high.reshape(count, HALF).astype(jnp.bfloat16)

    def project(weight):
        return jnp.dot(low, weight[:HALF], preferred_element_type=f32) + jnp.dot(
            high, weight[HALF:], preferred_element_type=f32
        )

    inner = []
    for gate_w, up_w in ((gate_a, up_a), (gate_b, up_b)):
        gate = project(gate_w)
        inner.append((gate / (1.0 + jnp.exp(-gate)) * project(up_w)).astype(jnp.bfloat16))
    halves = []
    for j in range(2):
        columns = slice(j * HALF, (j + 1) * HALF)
        half = jnp.dot(inner[0], down_a[:, columns], preferred_element_type=f32) + jnp.dot(
            inner[1], down_b[:, columns], preferred_element_type=f32
        )
        halves.append(half.reshape(sources // 2, 1, ROWS, HALF))
    first, second = swap_halves(jnp.concatenate(halves, axis=1))
    result[...] = (
        jnp.stack([first, second], axis=1).reshape(sources, ROWS, HALF).astype(jnp.bfloat16)
    )


def expert(rows, *weights):
    return pl.pallas_call(
        expert_kernel,
        out_shape=jax.ShapeDtypeStruct(rows.shape, rows.dtype),
        compiler_params=pltpu.CompilerParams(vmem_limit_bytes=32 * MIB),
        cost_estimate=pl.CostEstimate(
            flops=3_000_000_000, transcendentals=0, bytes_accessed=8 * MIB
        ),
        name="expert",
    )(rows, *weights)


def combine_kernel(returned, residual, weighting, out):
    count = residual.shape[0]
    values = returned[...].reshape(returned.shape[0] * ROWS, HALF)
    both = jnp.dot(weighting[...], values, preferred_element_type=jnp.float32)
    routed = both[: 2 * count] + both[2 * count :]
    res = residual[...].astype(jnp.float32)
    out[:, :HALF] = (res[:, :HALF] + routed[:count]).astype(jnp.bfloat16)
    out[:, HALF:] = (res[:, HALF:] + routed[count:]).astype(jnp.bfloat16)


def combine(returned, residual, weighting):
    return pl.pallas_call(
        combine_kernel,
        out_shape=jax.ShapeDtypeStruct(residual.shape, residual.dtype),
        compiler_params=pltpu.CompilerParams(vmem_limit_bytes=16 * MIB),
        name="combine",
    )(returned, residual, weighting)


def per_device(
    hidden,
    cache_keys,
    cache_values,
    lengths,
    first_gain,
    query_weight,
    key_weight,
    value_weight,
    mixing,
    head_gain,
    out_weight,
    second_gain,
    routes,
    route_weight,
    expert_gate,
    expert_up,
    expert_down,
):
    devices = lax.axis_size("ep")
    experts = devices // EXP_SPLIT
    partners = [(i, i ^ 1) for i in range(devices)]
    lanes = [[e * EXP_SPLIT + j for e in range(experts)] for j in range(EXP_SPLIT)]
    peer = [lax.ppermute(w[0], "ep", partners) for w in (expert_gate, expert_up, expert_down)]

    packed, residual, new_key, new_value, weighting = front(
        lengths,
        mixing,
        hidden,
        first_gain,
        head_gain,
        second_gain,
        routes,
        route_weight,
        query_weight,
        key_weight,
        value_weight,
        out_weight,
        cache_keys,
        cache_values,
        experts,
    )
    rows = lax.all_to_all(packed, "ep", 0, 0, axis_index_groups=lanes, tiled=True)
    result = expert(
        rows, expert_gate[0], peer[0], expert_up[0], peer[1], expert_down[0], peer[2]
    )
    returned = lax.all_to_all(result, "ep", 0, 0, axis_index_groups=lanes, tiled=True)
    layer_out = combine(returned, residual, weighting)
    return (layer_out, new_key, new_value)


def solution(mesh):
    return jax.shard_map(
        per_device,
        mesh=mesh,
        in_specs=(
            P("ep", None),
            P("ep", None, None),
            P("ep", None, None),
            P("ep"),
            P(),
            P(),
            P(),
            P(),
            P(),
            P(),
            P(),
            P(),
            P("ep", None),
            P("ep", None),
            P("ep", None, None),
            P("ep", None, None),
            P("ep", None, None),
        ),
        out_specs=(P("ep", None), P("ep", None), P("ep", None)),
        check_vma=False,
    )
```

```python
import jax
import jax.numpy as jnp
from jax import lax
from jax.experimental import pallas as pl
from jax.experimental.pallas import tpu as pltpu
from jax.sharding import PartitionSpec as P

D = 2048
HALF = D // 2
HEADS = 8
DK = 64
DV = 128
EXP_SPLIT = 2
TOP_K = 4
CAP = 4
ROWS = 8
BLOCK = 256
GROUP = 16
WCHUNKS = 4

epsilon = 1e-06
MIB = 1024 * 1024


def root_factor(values):
    return lax.rsqrt(jnp.mean(values * values, axis=-1, keepdims=True) + epsilon)


def routing_tables(routes, route_weight, pick, weighting_out):
    count = routes.shape[1]
    slots = pick.shape[0]
    f32 = jnp.float32
    across = [routes[j : j + 1, :].astype(f32) for j in range(TOP_K)]
    rows_at = lax.broadcasted_iota(jnp.int32, (count, count), 0)
    columns_at = lax.broadcasted_iota(jnp.int32, (count, count), 1)

    def turn(row):
        return jnp.sum(jnp.where(rows_at == columns_at, row, 0.0), axis=1, keepdims=True)

    down = [turn(row) for row in across]
    same = down[0] == across[0]
    for j in range(1, TOP_K):
        same = same | (down[0] == across[j])
    shared = jnp.where(same, 1.0, 0.0)
    rank_across = jnp.sum(jnp.where(rows_at < columns_at, shared, 0.0), axis=0, keepdims=True)
    rank_down = turn(rank_across)

    slot = lax.broadcasted_iota(jnp.int32, (slots, count), 0)
    expert = (slot // ROWS).astype(f32)
    hit = expert == across[0]
    for j in range(1, TOP_K):
        hit = hit | (expert == across[j])
    chosen = jnp.where(hit & ((slot % CAP).astype(f32) == rank_across), 1.0, 0.0)
    upper = (slot // CAP) % 2 == 1
    pick[...] = jnp.concatenate(
        [jnp.where(upper, 0.0, chosen), jnp.where(upper, chosen, 0.0)], axis=1
    ).astype(jnp.bfloat16)

    slot = lax.broadcasted_iota(jnp.int32, (count, slots), 1)
    expert = (slot // ROWS).astype(f32)
    weighting = jnp.zeros((count, slots), f32)
    for j in range(TOP_K):
        weighting = weighting + jnp.where(
            expert == down[j], turn(route_weight[j : j + 1, :]), 0.0
        )
    weighting = jnp.where((slot % CAP).astype(f32) == rank_down, weighting, 0.0)
    upper = (slot // CAP) % 2 == 1
    whole = jnp.concatenate(
        [jnp.where(upper, 0.0, weighting), jnp.where(upper, weighting, 0.0)], axis=0
    )
    coarse = whole.astype(jnp.bfloat16)
    fine = (whole - coarse.astype(f32)).astype(jnp.bfloat16)
    weighting_out[...] = jnp.concatenate([coarse, fine], axis=0)


def front_kernel(
    lengths_hbm,
    mixing_hbm,
    hidden_hbm,
    first_gain_hbm,
    head_gain_hbm,
    second_gain_hbm,
    routes_hbm,
    route_weight_hbm,
    wq_hbm,
    wk_hbm,
    wv_hbm,
    wo_hbm,
    keys_hbm,
    values_hbm,
    packed,
    residual_out,
    new_key_out,
    new_value_out,
    weighting_out,
    lengths,
    mixing,
    hidden,
    first_gain,
    head_gain,
    second_gain,
    routes,
    route_weight,
    wq,
    wk,
    wv,
    wo,
    kbuf,
    vbuf,
    queries,
    own_key,
    own_value,
    mixed,
    own_scores,
    scores_at,
    pick,
    order,
    ssem,
    wsem,
    osem,
    ksem,
    vsem,
):
    count = hidden.shape[0]
    span = keys_hbm.shape[1]
    blocks = span // BLOCK
    groups = count // GROUP
    part = D // WCHUNKS

    def weight_copies(i):
        rows = pl.ds(i * part, part)
        return [
            pltpu.make_async_copy(source.at[rows], target.at[rows], wsem.at[n, i])
            for n, (source, target) in enumerate(((wq_hbm, wq), (wk_hbm, wk), (wv_hbm, wv)))
        ]

    small = [
        pltpu.make_async_copy(source, target, ssem.at[n])
        for n, (source, target) in enumerate(
            (
                (lengths_hbm, lengths),
                (hidden_hbm, hidden),
                (first_gain_hbm, first_gain),
                (routes_hbm, routes),
                (route_weight_hbm, route_weight),
                (mixing_hbm, mixing),
                (head_gain_hbm, head_gain),
                (second_gain_hbm, second_gain),
            )
        )
    ]
    for copy in small:
        copy.start()
    for i in range(WCHUNKS):
        for copy in weight_copies(i):
            copy.start()
    small[0].wait()

    def passed(i):
        return [(lengths[i] > b * BLOCK).astype(jnp.int32) for b in range(1, blocks)]

    starts = [jnp.int32(0)] + [jnp.int32(count)] * (blocks - 1)
    for i in range(count):
        more = passed(i)
        starts = starts[:1] + [at - one for at, one in zip(starts[1:], more)]
    for i in range(count):
        more = passed(i)
        place = starts[0]
        for at, one in zip(starts[1:], more):
            place = jnp.where(one > 0, at, place)
        order[place] = jnp.int32(i)
        kinds = [1] + more + [0]
        starts = [at + (kinds[b] - kinds[b + 1]) for b, at in enumerate(starts)]

    def group_blocks(g):
        return 1 + sum(passed(order[g * GROUP + GROUP - 1]))

    def cache_copies(source, target, sem, g, n):
        rows = pl.ds(0, n * BLOCK)
        return [
            pltpu.make_async_copy(
                source.at[order[g * GROUP + i], rows],
                target.at[g * GROUP + i, rows],
                sem.at[g * GROUP + i],
            )
            for i in range(GROUP)
        ]

    def by_blocks(body):
        def step(g, carry):
            need = group_blocks(g)
            for n in range(1, blocks + 1):

                @pl.when(need == n)
                def _():
                    body(g, n)

            return carry

        lax.fori_loop(0, groups, step, 0)

    def start_keys(g, n):
        for copy in cache_copies(keys_hbm, kbuf, ksem, g, n):
            copy.start()

    def start_values(g, n):
        for copy in cache_copies(values_hbm, vbuf, vsem, g, n):
            copy.start()

    by_blocks(start_keys)
    by_blocks(start_values)
    wo_copy = pltpu.make_async_copy(wo_hbm, wo, osem)
    wo_copy.start()
    for copy in small[1:]:
        copy.wait()
    routing_tables(routes, route_weight, pick, weighting_out)

    hid = hidden[...].astype(jnp.float32)
    normed = (hid * root_factor(hid) * first_gain[...]).astype(jnp.bfloat16)
    q = jnp.zeros((count, HEADS * 2 * DK), jnp.float32)
    k = jnp.zeros((count, 2 * DK), jnp.float32)
    v = jnp.zeros((count, DV), jnp.float32)
    for i in range(WCHUNKS):
        for copy in weight_copies(i):
            copy.wait()
        rows = slice(i * part, (i + 1) * part)
        left = normed[:, rows]
        q = q + jnp.dot(left, wq[rows], preferred_element_type=jnp.float32)
        k = k + jnp.dot(left, wk[rows], preferred_element_type=jnp.float32)
        v = v + jnp.dot(left, wv[rows], preferred_element_type=jnp.float32)
    q = q.astype(jnp.bfloat16).astype(jnp.float32) * DK ** (-0.5)
    k = k.astype(jnp.bfloat16)
    v = v.astype(jnp.bfloat16)
    new_key_out[...] = k
    new_value_out[...] = v
    own_key[...] = k.astype(jnp.float32)
    own_value[...] = v.astype(jnp.float32)
    for h in range(HEADS):
        queries[pl.ds(h, count, stride=HEADS), :] = q[:, h * 2 * DK : (h + 1) * 2 * DK]

    head_at = lax.broadcasted_iota(jnp.int32, (HEADS, 1), 0)
    mix = jnp.zeros((HEADS, 1), jnp.float32)
    for h in range(HEADS):
        mix = jnp.where(head_at == h, mixing[h], mix)
    low = lax.broadcasted_iota(jnp.int32, (HEADS, 2 * DK), 1) < DK
    pair = 2 * HEADS
    lane_owner = lax.broadcasted_iota(jnp.int32, (2 * DK, GROUP * pair), 1) // pair

    def score_group(g, n):
        wide = n * BLOCK
        both = []
        for i in range(GROUP):
            s = order[g * GROUP + i]
            rows = queries[pl.ds(pl.multiple_of(s * HEADS, HEADS), HEADS), :]
            both.append(
                jnp.concatenate([jnp.where(low, rows, 0.0), jnp.where(low, 0.0, rows)], axis=0)
            )
            own_rows = both[i] * own_key[pl.ds(s, 1), :]
            own_scores[g, i * pair : (i + 1) * pair, :] = own_rows
        turned = jnp.concatenate(both, axis=0).T
        spread = jnp.concatenate(
            [jnp.where(lane_owner == i, turned, 0.0) for i in range(GROUP)], axis=0
        ).astype(jnp.bfloat16)
        for copy in cache_copies(keys_hbm, kbuf, ksem, g, n):
            copy.wait()
        keys = jnp.concatenate([kbuf[g * GROUP + i, :wide, :] for i in range(GROUP)], axis=1)
        scores_at[g, :, :wide] = jnp.dot(keys, spread, preferred_element_type=jnp.float32).T

    def mix_group(g, n):
        wide = n * BLOCK
        column = lax.broadcasted_iota(jnp.int32, (pair, wide), 1)
        for copy in cache_copies(values_hbm, vbuf, vsem, g, n):
            copy.wait()
        for i in range(GROUP):
            s = order[g * GROUP + i]
            rows = slice(i * pair, (i + 1) * pair)
            own = jnp.sum(own_scores[g, rows, :], axis=-1, keepdims=True)
            scores = jnp.where(column < lengths[s], scores_at[g, rows, :wide], -jnp.inf)
            highest = jnp.maximum(jnp.max(scores, axis=-1, keepdims=True), own)
            weights = jnp.exp(scores - highest)
            own_weights = jnp.exp(own - highest)
            total = jnp.sum(weights, axis=-1, keepdims=True) + own_weights
            first = 1.0 / total[:HEADS]
            second = mix / total[HEADS:]
            contrast = (weights[:HEADS] * first - weights[HEADS:] * second).astype(jnp.bfloat16)
            own_contrast = (own_weights[:HEADS] * first - own_weights[HEADS:] * second).astype(
                jnp.bfloat16
            )
            out = jnp.dot(
                contrast, vbuf[g * GROUP + i, :wide, :], preferred_element_type=jnp.float32
            )
            out = out + own_contrast.astype(jnp.float32) * own_value[pl.ds(s, 1), :]
            mixed[pl.ds(pl.multiple_of(s * HEADS, HEADS), HEADS), :] = out

    by_blocks(score_group)
    by_blocks(mix_group)

    pieces = []
    for h in range(HEADS):
        rows = mixed[pl.ds(h, count, stride=HEADS), :]
        pieces.append((rows * root_factor(rows) * head_gain[...]).astype(jnp.bfloat16))
    head_rows = jnp.concatenate(pieces, axis=1)
    wo_copy.wait()
    update = jnp.dot(head_rows, wo[...], preferred_element_type=jnp.float32)
    residual = (hid + update).astype(jnp.bfloat16)
    residual_out[...] = residual
    res = residual.astype(jnp.float32)
    expert_input = (res * root_factor(res) * second_gain[...]).astype(jnp.bfloat16)

    stacked = jnp.concatenate([expert_input[:, :HALF], expert_input[:, HALF:]], axis=0)
    sent = jnp.dot(pick[...], stacked, preferred_element_type=jnp.float32).astype(jnp.bfloat16)
    packed[...] = sent.reshape(packed.shape)


def front(
    lengths,
    mixing,
    hidden,
    first_gain,
    head_gain,
    second_gain,
    routes,
    route_weight,
    wq,
    wk,
    wv,
    wo,
    keys,
    values,
    experts,
):
    count = hidden.shape[0]
    slots = experts * ROWS
    vmem = pl.BlockSpec(memory_space=pltpu.VMEM)
    hbm = pl.BlockSpec(memory_space=pltpu.HBM)
    bf16 = jnp.bfloat16
    f32 = jnp.float32
    operands = (
        lengths,
        mixing,
        hidden,
        first_gain.reshape(1, D),
        head_gain.reshape(1, DV),
        second_gain.reshape(1, D),
        routes.T,
        route_weight.T,
        wq,
        wk,
        wv,
        wo,
        keys,
        values,
    )
    return pl.pallas_call(
        front_kernel,
        out_shape=(
            jax.ShapeDtypeStruct((experts, ROWS, HALF), bf16),
            jax.ShapeDtypeStruct((count, D), bf16),
            jax.ShapeDtypeStruct((count, 2 * DK), bf16),
            jax.ShapeDtypeStruct((count, DV), bf16),
            jax.ShapeDtypeStruct((4 * count, slots), bf16),
        ),
        in_specs=[hbm] * 14,
        out_specs=(vmem,) * 5,
        scratch_shapes=[
            pltpu.SMEM(lengths.shape, jnp.int32),
            pltpu.SMEM(mixing.shape, f32),
            pltpu.VMEM(hidden.shape, bf16),
            pltpu.VMEM((1, D), f32),
            pltpu.VMEM((1, DV), f32),
            pltpu.VMEM((1, D), f32),
            pltpu.VMEM((TOP_K, count), jnp.int32),
            pltpu.VMEM((TOP_K, count), f32),
            pltpu.VMEM(wq.shape, bf16),
            pltpu.VMEM(wk.shape, bf16),
            pltpu.VMEM(wv.shape, bf16),
            pltpu.VMEM(wo.shape, bf16),
            pltpu.VMEM(keys.shape, bf16),
            pltpu.VMEM(values.shape, bf16),
            pltpu.VMEM((count * HEADS, 2 * DK), f32),
            pltpu.VMEM((count, 2 * DK), f32),
            pltpu.VMEM((count, DV), f32),
            pltpu.VMEM((count * HEADS, DV), f32),
            pltpu.VMEM((count // GROUP, GROUP * 2 * HEADS, 2 * DK), f32),
            pltpu.VMEM((count // GROUP, GROUP * 2 * HEADS, keys.shape[1]), f32),
            pltpu.VMEM((slots, 2 * count), bf16),
            pltpu.SMEM((count + 1,), jnp.int32),
            pltpu.SemaphoreType.DMA((8,)),
            pltpu.SemaphoreType.DMA((3, WCHUNKS)),
            pltpu.SemaphoreType.DMA(()),
            pltpu.SemaphoreType.DMA((count,)),
            pltpu.SemaphoreType.DMA((count,)),
        ],
        compiler_params=pltpu.CompilerParams(vmem_limit_bytes=40 * MIB),
        cost_estimate=pl.CostEstimate(
            flops=20_000_000_000, transcendentals=0, bytes_accessed=25 * MIB
        ),
        name="front",
    )(*[pltpu.with_memory_space_constraint(x, pltpu.HBM) for x in operands])


def swap_halves(pairs):
    first = pairs[:, 0]
    second = pairs[:, 1]
    top = lax.broadcasted_iota(jnp.int32, first.shape, 1) < CAP
    low = jnp.where(top, first, pltpu.roll(second, CAP, 1))
    high = jnp.where(top, pltpu.roll(first, CAP, 1), second)
    return low, high


def expert_kernel(rows, gate_a, gate_b, up_a, up_b, down_a, down_b, result):
    sources = rows.shape[0]
    count = sources * CAP
    f32 = jnp.float32
    pairs = rows[...].astype(f32).reshape(sources // 2, 2, ROWS, HALF)
    low, high = swap_halves(pairs)
    low = low.reshape(count, HALF).astype(jnp.bfloat16)
    high = high.reshape(count, HALF).astype(jnp.bfloat16)

    def project(weight):
        return jnp.dot(low, weight[:HALF], preferred_element_type=f32) + jnp.dot(
            high, weight[HALF:], preferred_element_type=f32
        )

    inner = []
    for gate_w, up_w in ((gate_a, up_a), (gate_b, up_b)):
        gate = project(gate_w)
        inner.append((gate / (1.0 + jnp.exp(-gate)) * project(up_w)).astype(jnp.bfloat16))
    halves = []
    for j in range(2):
        columns = slice(j * HALF, (j + 1) * HALF)
        half = jnp.dot(inner[0], down_a[:, columns], preferred_element_type=f32) + jnp.dot(
            inner[1], down_b[:, columns], preferred_element_type=f32
        )
        halves.append(half.reshape(sources // 2, 1, ROWS, HALF))
    first, second = swap_halves(jnp.concatenate(halves, axis=1))
    result[...] = (
        jnp.stack([first, second], axis=1).reshape(sources, ROWS, HALF).astype(jnp.bfloat16)
    )


def expert(rows, *weights):
    return pl.pallas_call(
        expert_kernel,
        out_shape=jax.ShapeDtypeStruct(rows.shape, rows.dtype),
        compiler_params=pltpu.CompilerParams(vmem_limit_bytes=32 * MIB),
        cost_estimate=pl.CostEstimate(
            flops=3_000_000_000, transcendentals=0, bytes_accessed=8 * MIB
        ),
        name="expert",
    )(rows, *weights)


def combine_kernel(returned, residual, weighting, out):
    count = residual.shape[0]
    values = returned[...].reshape(returned.shape[0] * ROWS, HALF)
    both = jnp.dot(weighting[...], values, preferred_element_type=jnp.float32)
    routed = both[: 2 * count] + both[2 * count :]
    res = residual[...].astype(jnp.float32)
    out[:, :HALF] = (res[:, :HALF] + routed[:count]).astype(jnp.bfloat16)
    out[:, HALF:] = (res[:, HALF:] + routed[count:]).astype(jnp.bfloat16)


def combine(returned, residual, weighting):
    return pl.pallas_call(
        combine_kernel,
        out_shape=jax.ShapeDtypeStruct(residual.shape, residual.dtype),
        compiler_params=pltpu.CompilerParams(vmem_limit_bytes=16 * MIB),
        name="combine",
    )(returned, residual, weighting)


def per_device(
    hidden,
    cache_keys,
    cache_values,
    lengths,
    first_gain,
    query_weight,
    key_weight,
    value_weight,
    mixing,
    head_gain,
    out_weight,
    second_gain,
    routes,
    route_weight,
    expert_gate,
    expert_up,
    expert_down,
):
    devices = lax.axis_size("ep")
    experts = devices // EXP_SPLIT
    partners = [(i, i ^ 1) for i in range(devices)]
    lanes = [[e * EXP_SPLIT + j for e in range(experts)] for j in range(EXP_SPLIT)]
    peer = [lax.ppermute(w[0], "ep", partners) for w in (expert_gate, expert_up, expert_down)]

    packed, residual, new_key, new_value, weighting = front(
        lengths,
        mixing,
        hidden,
        first_gain,
        head_gain,
        second_gain,
        routes,
        route_weight,
        query_weight,
        key_weight,
        value_weight,
        out_weight,
        cache_keys,
        cache_values,
        experts,
    )
    rows = lax.all_to_all(packed, "ep", 0, 0, axis_index_groups=lanes, tiled=True)
    result = expert(
        rows, expert_gate[0], peer[0], expert_up[0], peer[1], expert_down[0], peer[2]
    )
    returned = lax.all_to_all(result, "ep", 0, 0, axis_index_groups=lanes, tiled=True)
    layer_out = combine(returned, residual, weighting)
    return (layer_out, new_key, new_value)


def solution(mesh):
    return jax.shard_map(
        per_device,
        mesh=mesh,
        in_specs=(
            P("ep", None),
            P("ep", None, None),
            P("ep", None, None),
            P("ep"),
            P(),
            P(),
            P(),
            P(),
            P(),
            P(),
            P(),
            P(),
            P("ep", None),
            P("ep", None),
            P("ep", None, None),
            P("ep", None, None),
            P("ep", None, None),
        ),
        out_specs=(P("ep", None), P("ep", None), P("ep", None)),
        check_vma=False,
    )
```
